32 devices in a mesh: grp: 2 (over y), sp: 4 (over z), tp: 4 (over x, core).
Axes of the slice: x: 2, y: 2, z: 4, core: 2. Of those that a mesh axis runs over, the one named last changes fastest.
Arguments:
- residual_in: bfloat16 [2048, 2048], P(('grp', 'sp', 'tp')), parts along dimension 0, may hold values from -6 to 6
- query_rows: bfloat16 [2048, 2048], P(('grp', 'sp'), 'tp'), parts along dimension 0, may hold values from -6 to 6
- key_rows: bfloat16 [2048, 512], P(('grp', 'sp'), 'tp'), parts along dimension 0, may hold values from -6 to 6
- value_rows: bfloat16 [2048, 512], P(('grp', 'sp'), 'tp'), parts along dimension 0, may hold values from -6 to 6
- forget_cumsum: float32 [2048, 16], P(('grp', 'sp'), 'tp'), parts along dimension 0, as said below
- head_gain: float32 [2048], P('tp'), may hold values from 0.1 to 1.9
- w_out: bfloat16 [2048, 2048], P('tp'), may hold values from -0.125 to 0.125
- w_up: bfloat16 [2048, 8192], P('sp', 'tp'), may hold values from -0.125 to 0.125
- w_down: bfloat16 [8192, 2048], P('tp', 'sp'), may hold values from -0.0625 to 0.0625
- mixer_gain: float32 [2048], replicated, may hold values from 0.1 to 1.9
- channel_gain: float32 [2048], replicated, may hold values from 0.1 to 1.9
Outputs:
- layer_out: bfloat16 [2048, 2048], P(('grp', 'sp', 'tp')), parts along dimension 0
The draws below stay inside these ranges and needn't reach their ends.
There are 2 independent parts, one for each index of `grp`. The reference program is written for one: setup_inputs(seed, part) draws one part's arguments, and reference() takes and returns one part's arrays. A program takes and returns all parts, laid end to end along the dimension named above; an argument that names none is the same for every part. Nothing has to cross between parts.
Inputs may be any that keep to these rules, and one draw needn't show every extreme that they name: `forget_cumsum`: Non-positive; along the positions, each head's entries never rise.
All inputs are finite; a program needn't handle non-finite values.
Results may differ from the reference program's by a relative error of at most 0.015.
Values may be sent and summed in bfloat16 or wider, within the bound.
A program may use at most 128 MiB of HBM per device.

```python
import jax
import jax.numpy as jnp
from jax import lax

D = 2048
QUERY_HEADS = 16
KV_HEADS = 4
HD = 128
FF = 8192
TOK_DEV = 256
SEQUENCE_TOKENS = 1024


def draw_key_rows(key, part):
    drawn = jax.random.normal(jax.random.fold_in(key, 21), (SEQUENCE_TOKENS, KV_HEADS * HD), jnp.float32)
    drawn = jnp.clip(drawn, -6.0, 6.0)
    return drawn.astype(jnp.bfloat16)


def draw_query_rows(key, part):
    drawn = jax.random.normal(jax.random.fold_in(key, 22), (SEQUENCE_TOKENS, QUERY_HEADS * HD), jnp.float32)
    drawn = jnp.clip(drawn, -6.0, 6.0)
    return drawn.astype(jnp.bfloat16)


def draw_forget_cumsum(key, part):
    residual_paths = [jax.random.fold_in(key, 30 + offset) for offset in range(7)]
    slow_share = 0.5
    sluggish_part = jax.random.uniform(residual_paths[0], (QUERY_HEADS,)) < slow_share
    slow_total = jax.random.uniform(residual_paths[1], (QUERY_HEADS,), minval=0.1, maxval=0.5)
    fast_rate = 1.0 / jax.random.uniform(residual_paths[2], (QUERY_HEADS,), minval=30.0, maxval=100.0)
    rate = jnp.where(sluggish_part, slow_total / SEQUENCE_TOKENS, fast_rate)
    position = jnp.arange(SEQUENCE_TOKENS, dtype=jnp.float32)
    ramp = 0.5 + position / SEQUENCE_TOKENS
    block_factor = jnp.exp(jax.random.uniform(residual_paths[3], (SEQUENCE_TOKENS // TOK_DEV,), minval=-0.7, maxval=0.7))
    block_factor = jnp.repeat(block_factor, TOK_DEV)
    rough = jax.random.uniform(residual_paths[4], (SEQUENCE_TOKENS, QUERY_HEADS), minval=0.2, maxval=1.8)
    gate_logarithm = -rate[None, :] * (ramp * block_factor)[:, None] * rough
    spike_position = jax.random.randint(residual_paths[5], (3,), 0, SEQUENCE_TOKENS)
    spike_penalty = jax.random.uniform(residual_paths[6], (3, QUERY_HEADS), minval=0.2, maxval=0.5)
    matched_rows = (jnp.arange(SEQUENCE_TOKENS)[:, None] == spike_position[None, :]).astype(jnp.float32)
    spike_pattern = jnp.dot(matched_rows, jnp.log(1.0 - spike_penalty))
    gate_logarithm = gate_logarithm + jnp.where(sluggish_part[None, :], spike_pattern, 0.0)
    return jnp.cumsum(gate_logarithm, axis=0).astype(jnp.float32)


def steps_of(stream_key, shape, cuts, least, largest):
    loudness, own = 1.0, jax.random.fold_in(stream_key, 6)
    for dim, shards_of in cuts:
        draws = jnp.exp(jax.random.uniform(jax.random.fold_in(own, dim), (shards_of,), jnp.float32, least / len(cuts), largest / len(cuts)))
        loudness = loudness * jnp.repeat(draws, shape[dim] // shards_of).reshape([-1 if axis == dim else 1 for axis in range(len(shape))])
    return loudness


def scatter_about(own_key, extent, width, most, pieces=(), held_as=jnp.bfloat16):
    values = width * jax.random.normal(own_key, extent, jnp.float32)
    if pieces:
        values = values * steps_of(own_key, extent, pieces, -0.22, 0.18)
    return jnp.clip(values, -most, most).astype(held_as)


def setup_inputs(seed: int = 0, part: int = 0) -> dict:
    splits = jax.random.split(jax.random.key(seed), 12)
    own_keys = jax.random.split(jax.random.fold_in(splits[11], part), 12)
    residual_in = scatter_about(own_keys[0], (SEQUENCE_TOKENS, D), 1.0, 6.0, ((0, 16),))
    query_rows = draw_query_rows(jax.random.fold_in(jax.random.fold_in(splits[11], part), 71), part)
    key_rows = draw_key_rows(jax.random.fold_in(jax.random.fold_in(splits[11], part), 71), part)
    value_rows = scatter_about(own_keys[3], (SEQUENCE_TOKENS, KV_HEADS * HD), 1.0, 6.0, ((0, 4), (1, 4)))
    forget_cumsum = draw_forget_cumsum(jax.random.fold_in(jax.random.fold_in(splits[11], part), 71), part)
    head_gain = jnp.clip(1.0 + 0.18 * jax.random.normal(splits[5], (QUERY_HEADS * HD,), jnp.float32), 0.1, 1.9)
    w_out = scatter_about(splits[6], (QUERY_HEADS * HD, D), (QUERY_HEADS * HD) ** -0.5, 0.125, ((0, 4),))
    w_up = scatter_about(splits[7], (D, FF), D ** -0.5, 0.125, ((0, 4), (1, 4)))
    w_down = scatter_about(splits[8], (FF, D), FF ** -0.5, 0.0625, ((0, 4), (1, 4)))
    mixer_gain = jnp.clip(1.0 + 0.18 * jax.random.normal(splits[9], (D,), jnp.float32), 0.1, 1.9)
    channel_gain = jnp.clip(1.0 + 0.18 * jax.random.normal(splits[10], (D,), jnp.float32), 0.1, 1.9)
    return {"residual_in": residual_in, "query_rows": query_rows, "key_rows": key_rows, "value_rows": value_rows, "forget_cumsum": forget_cumsum, "head_gain": head_gain, "w_out": w_out, "w_up": w_up, "w_down": w_down, "mixer_gain": mixer_gain, "channel_gain": channel_gain}


ALPHA = 8.0 ** 0.25
EPSILON = 1e-05
NEG_FILL = -1e+30

def layer_scale(inputs, gain_vec):
    centered = inputs - lax.optimization_barrier(jnp.mean(inputs, axis=-1, keepdims=True))
    variance = lax.optimization_barrier(jnp.mean(centered * centered, axis=-1, keepdims=True))
    return centered * lax.rsqrt(variance + EPSILON) * gain_vec

def reference(residual_in, query_rows, key_rows, value_rows, forget_cumsum, head_gain, w_out, w_up, w_down, mixer_gain, channel_gain):
    group_size = QUERY_HEADS // KV_HEADS
    block_rows = 512 if SEQUENCE_TOKENS % 512 == 0 else SEQUENCE_TOKENS
    block_count = SEQUENCE_TOKENS // block_rows
    score_scale = HD ** (-0.5)
    key_full = key_rows.astype(jnp.float32).reshape(SEQUENCE_TOKENS, KV_HEADS, HD)
    value_full = value_rows.astype(jnp.float32).reshape(SEQUENCE_TOKENS, KV_HEADS, HD)
    gate_keys = forget_cumsum.reshape(SEQUENCE_TOKENS, KV_HEADS, group_size).transpose(1, 2, 0)
    key_pos = jnp.arange(SEQUENCE_TOKENS, dtype=jnp.int32)

    def attend(block_index):
        first_row = (block_index * block_rows).astype(jnp.int32)
        query_full = lax.dynamic_slice_in_dim(query_rows, first_row, block_rows, 0).astype(jnp.float32)
        query_full = query_full.reshape(block_rows, KV_HEADS, group_size, HD)
        gate_rows = lax.dynamic_slice_in_dim(forget_cumsum, first_row, block_rows, 0)
        gate_rows = gate_rows.reshape(block_rows, KV_HEADS, group_size).transpose(1, 2, 0)
        scores = jnp.einsum('tkgd,ukd->kgtu', query_full, key_full) * score_scale
        scores = scores + gate_rows[..., None] - gate_keys[:, :, None, :]
        query_pos = first_row + jnp.arange(block_rows, dtype=jnp.int32)
        allowed = key_pos[None, :] <= query_pos[:, None]
        scores = jnp.where(allowed, scores, NEG_FILL)
        peak_score = lax.optimization_barrier(jnp.max(scores, axis=-1, keepdims=True))
        weights = jnp.exp(scores - peak_score)
        denom_sum = lax.optimization_barrier(jnp.sum(weights, axis=-1))
        rounded = lax.optimization_barrier(weights.astype(jnp.bfloat16)).astype(jnp.float32)
        attended = jnp.einsum('kgtu,ukd->kgtd', rounded, value_full) / denom_sum[..., None]
        normed = attended * lax.rsqrt(lax.optimization_barrier(jnp.mean(attended * attended, axis=-1, keepdims=True)) + EPSILON)
        normed = normed * head_gain.reshape(KV_HEADS, group_size, 1, HD)
        return normed.transpose(2, 0, 1, 3).reshape(block_rows, QUERY_HEADS * HD).astype(jnp.bfloat16)
    heads_out = lax.map(attend, jnp.arange(block_count, dtype=jnp.int32)).reshape(SEQUENCE_TOKENS, QUERY_HEADS * HD)
    branch = jnp.dot(heads_out, w_out, preferred_element_type=jnp.float32)
    mid = layer_scale(ALPHA * residual_in.astype(jnp.float32) + branch, mixer_gain).astype(jnp.bfloat16)
    lifted = jnp.dot(mid, w_up, preferred_element_type=jnp.float32)
    active = jnp.square(jax.nn.relu(lifted)).astype(jnp.bfloat16)
    lowered = jnp.dot(active, w_down, preferred_element_type=jnp.float32)
    return layer_scale(ALPHA * mid.astype(jnp.float32) + lowered, channel_gain).astype(jnp.bfloat16)
```

```python
import functools

import jax
import jax.numpy as jnp
from jax import lax
from jax.experimental import pallas as pl
from jax.experimental.pallas import tpu as pltpu
from jax.sharding import PartitionSpec as P

MESH = pl.DeviceIdType.MESH

HD = 128


ALPHA = 8.0**0.25
EPSILON = 1e-05
NEG_FILL = -1e30


def layer_scale(inputs, gain_vec):
    centered = inputs - jnp.mean(inputs, axis=-1, keepdims=True)
    variance = jnp.mean(centered * centered, axis=-1, keepdims=True)
    return centered * lax.rsqrt(variance + EPSILON) * gain_vec


def shards(
    residual_in,
    query_rows,
    key_rows,
    value_rows,
    forget_cumsum,
    head_gain,
    w_out,
    w_up,
    w_down,
    mixer_gain,
    channel_gain,
):
    tok_rows = query_rows.shape[0]
    heads_here = forget_cumsum.shape[1]
    kv_here = key_rows.shape[1] // HD
    group_size = heads_here // kv_here
    score_scale = HD ** (-0.5)
    seq_index = lax.axis_index("sp")
    gate_all = lax.all_gather(forget_cumsum, "sp", axis=0, tiled=True)
    query_grid = query_rows.reshape(tok_rows, kv_here, group_size, HD)
    query_pos = seq_index * tok_rows + jnp.arange(tok_rows, dtype=jnp.int32)
    last_query = seq_index * tok_rows + tok_rows - 1
    gate_query = forget_cumsum.reshape(tok_rows, kv_here, group_size).transpose(1, 2, 0)

    def attend(carry_state, key_block, value_block, first_row):
        row_count = key_block.shape[0]

        def attend_live(live_state):
            peak_score, denom_sum, accum = live_state
            key_grid = key_block.reshape(row_count, kv_here, HD)
            value_grid = value_block.reshape(row_count, kv_here, HD)
            gate_block = lax.dynamic_slice_in_dim(gate_all, first_row, row_count, 0)
            gate_block = gate_block.reshape(row_count, kv_here, group_size).transpose(1, 2, 0)
            scores = (
                jnp.einsum(
                    "tkgd,ukd->kgtu", query_grid, key_grid, preferred_element_type=jnp.float32
                )
                * score_scale
            )
            scores = scores + gate_query[..., None] - gate_block[:, :, None, :]
            key_pos = first_row + jnp.arange(row_count, dtype=jnp.int32)
            allowed = key_pos[None, :] <= query_pos[:, None]
            scores = jnp.where(allowed, scores, NEG_FILL)
            new_peak = jnp.maximum(peak_score, jnp.max(scores, axis=-1))
            weights = jnp.where(allowed, jnp.exp(scores - new_peak[..., None]), 0.0)
            fade_factor = jnp.exp(peak_score - new_peak)
            denom_sum = denom_sum * fade_factor + jnp.sum(weights, axis=-1)
            accum = accum * fade_factor[..., None] + jnp.einsum(
                "kgtu,ukd->kgtd",
                weights.astype(jnp.bfloat16),
                value_grid,
                preferred_element_type=jnp.float32,
            )
            return (new_peak, denom_sum, accum)

        return lax.cond(
            first_row <= last_query, attend_live, lambda kept_state: kept_state, carry_state
        )

    def fold_keys(carry_state, pieces, first_row):
        key_piece, value_piece = pieces
        row_count = key_piece.shape[0]
        block_span = 1024
        if row_count > block_span and row_count % block_span == 0:

            def scan_block(scan_state, block_index):
                offset = block_index * block_span
                next_state = attend(
                    scan_state,
                    lax.dynamic_slice_in_dim(key_piece, offset, block_span, 0),
                    lax.dynamic_slice_in_dim(value_piece, offset, block_span, 0),
                    first_row + offset,
                )
                return (next_state, None)

            carry_state, unused = lax.scan(
                scan_block, carry_state, jnp.arange(row_count // block_span, dtype=jnp.int32)
            )
            return carry_state
        return attend(carry_state, key_piece, value_piece, first_row)

    fold_init = (
        jnp.full((kv_here, group_size, tok_rows), NEG_FILL, jnp.float32),
        jnp.zeros((kv_here, group_size, tok_rows), jnp.float32),
        jnp.zeros((kv_here, group_size, tok_rows, HD), jnp.float32),
    )
    peak_score, denom_sum, accum = fold_keys(
        fold_init,
        (
            lax.all_gather(key_rows, "sp", axis=0, tiled=True),
            lax.all_gather(value_rows, "sp", axis=0, tiled=True),
        ),
        jnp.int32(0),
    )
    attended = accum / denom_sum[..., None]
    normed = attended * lax.rsqrt(jnp.mean(attended * attended, axis=-1, keepdims=True) + EPSILON)
    normed = normed * head_gain.reshape(kv_here, group_size, 1, HD)
    heads_out = normed.transpose(2, 0, 1, 3).reshape(tok_rows, heads_here * HD).astype(jnp.bfloat16)
    branch = lax.psum_scatter(
        jnp.dot(heads_out, w_out, preferred_element_type=jnp.float32).astype(jnp.bfloat16),
        "tp",
        scatter_dimension=0,
        tiled=True,
    ).astype(jnp.float32)
    mid_rows = layer_scale(ALPHA * residual_in.astype(jnp.float32) + branch, mixer_gain).astype(
        jnp.bfloat16
    )
    mid_all = lax.all_gather(mid_rows, "tp", axis=0, tiled=True)
    up_full, down_full = (
        lax.all_gather(w_up, "sp", axis=0, tiled=True),
        lax.all_gather(w_down, "sp", axis=1, tiled=True),
    )
    lifted = jnp.dot(mid_all, up_full, preferred_element_type=jnp.float32)
    active = jnp.square(jax.nn.relu(lifted)).astype(jnp.bfloat16)
    lowered = lax.psum_scatter(
        jnp.dot(active, down_full, preferred_element_type=jnp.float32).astype(jnp.bfloat16),
        "tp",
        scatter_dimension=0,
        tiled=True,
    ).astype(jnp.float32)
    return layer_scale(ALPHA * mid_rows.astype(jnp.float32) + lowered, channel_gain).astype(
        jnp.bfloat16
    )


def layer_kernel(
    G,
    S,
    T,
    q_ref,
    k_ref,
    v_ref,
    gq_ref,
    gk_ref,
    res_ref,
    hg_ref,
    mg_ref,
    cg_ref,
    wout_hbm,
    wup_hbm,
    wdn_hbm,
    out_ref,
    kbuf,
    vbuf,
    gbuf,
    wout,
    wup,
    wdn,
    heads_v,
    mid_all,
    act,
    send_a,
    recv_a,
    keep,
    send_b,
    recv_b,
    own,
    send_c,
    recv_c,
    st_m,
    st_l,
    st_o,
    kv_s,
    kv_r,
    wz_s,
    wz_r,
    wy_s,
    wy_r,
    loc,
    z_s,
    z_r,
    x_s,
    x_r,
    d_s,
    d_r,
    a_s,
    a_r,
    b_s,
    b_r,
    c_s,
    c_r,
):
    f32, bf16 = jnp.float32, jnp.bfloat16
    X = T // 2
    g, s, t = lax.axis_index("grp"), lax.axis_index("sp"), lax.axis_index("tp")
    x, c = t // 2, lax.rem(t, 2)
    mate = x * 2 + (1 - c)
    tok = q_ref.shape[0]
    heads = gq_ref.shape[1]
    kv_heads = k_ref.shape[1] // HD
    group = heads // kv_heads
    rows = tok // T
    half = X * rows
    D = res_ref.shape[1]
    dcut = D // S
    fcut = wup.shape[1]

    def remote(src, dst, ssem, rsem, **where):
        return pltpu.make_async_remote_copy(
            src_ref=src,
            dst_ref=dst,
            send_sem=ssem,
            recv_sem=rsem,
            device_id=where,
            device_id_type=MESH,
        )

    def at_x(xo):
        return xo * 2 + c

    others_s = [lax.rem(s + d, S) for d in range(1, S)]
    others_x = [lax.rem(x + d, X) for d in range(1, X)]
    others_g = [lax.rem(g + d, G) for d in range(1, G)]

    own_copies = [
        pltpu.make_async_copy(wout_hbm, wout, loc.at[0]),
        pltpu.make_async_copy(
            wup_hbm.at[:, pl.ds(pl.multiple_of(s * fcut, fcut), fcut)],
            wup.at[pl.ds(pl.multiple_of(s * dcut, dcut), dcut), :],
            loc.at[1],
        ),
        pltpu.make_async_copy(
            wdn_hbm.at[pl.ds(pl.multiple_of(s * fcut, fcut), fcut), :],
            wdn.at[:, pl.ds(pl.multiple_of(s * dcut, dcut), dcut)],
            loc.at[2],
        ),
    ]
    for copy in own_copies:
        copy.start()

    barrier = pltpu.get_barrier_semaphore()
    for so in others_s:
        pl.semaphore_signal(barrier, inc=1, device_id={"sp": so}, device_id_type=MESH)
    for xo in others_x:
        pl.semaphore_signal(barrier, inc=1, device_id={"tp": at_x(xo)}, device_id_type=MESH)
    pl.semaphore_signal(barrier, inc=1, device_id={"tp": mate}, device_id_type=MESH)
    for go in others_g:
        pl.semaphore_signal(barrier, inc=1, device_id={"grp": go}, device_id_type=MESH)
    pl.semaphore_wait(barrier, (S - 1) + (X - 1) + 1 + (G - 1))

    def kv_copies(d):
        to = lax.rem(s + d, S)
        return [
            remote(k_ref, kbuf.at[d], kv_s.at[d, 0], kv_r.at[d, 0], sp=to),
            remote(v_ref, vbuf.at[d], kv_s.at[d, 1], kv_r.at[d, 1], sp=to),
            remote(gk_ref, gbuf.at[d], kv_s.at[d, 2], kv_r.at[d, 2], sp=to),
        ]

    for d in range(1, S):

        @pl.when(s + d < S)
        def _(d=d):
            for copy in kv_copies(d):
                copy.start()

    uprow, dnrow = dcut // G, fcut // G

    def up_piece(so, go):
        return wup.at[pl.ds(pl.multiple_of(so * dcut + go * uprow, uprow), uprow), :]

    def dn_piece(so, go):
        return wdn.at[
            pl.ds(pl.multiple_of(go * dnrow, dnrow), dnrow),
            pl.ds(pl.multiple_of(so * dcut, dcut), dcut),
        ]

    def z_weight(m, to):
        if m == 0:
            src = wup_hbm.at[
                pl.ds(pl.multiple_of(g * uprow, uprow), uprow),
                pl.ds(pl.multiple_of(to * fcut, fcut), fcut),
            ]
            dst = up_piece(s, g)
        else:
            src = wdn_hbm.at[pl.ds(pl.multiple_of(to * fcut + g * dnrow, dnrow), dnrow), :]
            dst = dn_piece(s, g)
        return remote(src, dst, wz_s.at[m, to], wz_r.at[m, s], sp=to)

    def z_weight_in(m, so):
        dst = up_piece(so, g) if m == 0 else dn_piece(so, g)
        return remote(dst, dst, wz_s.at[m, so], wz_r.at[m, so], sp=so)

    def y_weight(m, so, go):
        ref = up_piece(so, g) if m == 0 else dn_piece(so, g)
        return remote(ref, ref, wy_s.at[m, so, go], wy_r.at[m, so, g], grp=go)

    def y_weight_in(m, so, go):
        ref = up_piece(so, go) if m == 0 else dn_piece(so, go)
        return remote(ref, ref, wy_s.at[m, so, go], wy_r.at[m, so, go], grp=go)

    def start_weight(m):
        for so in others_s:
            z_weight(m, so).start()

    def forward_weight(m):
        for so in others_s:
            z_weight_in(m, so).wait_recv()
            for go in others_g:
                y_weight(m, so, go).start()

    def finish_weight(m):
        for so in others_s:
            for go in others_g:
                y_weight_in(m, so, go).wait_recv()

    start_weight(0)
    start_weight(1)

    scale = HD ** (-0.5)
    nt = (((1,), (1,)), ((), ()))
    tri = lax.broadcasted_iota(jnp.int32, (tok, tok), 0) >= lax.broadcasted_iota(
        jnp.int32, (tok, tok), 1
    )
    for h in range(heads):
        kh = h // group
        sc = lax.dot_general(
            q_ref[:, h * HD : (h + 1) * HD],
            k_ref[:, kh * HD : (kh + 1) * HD],
            nt,
            preferred_element_type=f32,
        )
        sc = sc * scale + gq_ref[:, h : h + 1] - gk_ref[h : h + 1, :]
        sc = jnp.where(tri, sc, NEG_FILL)
        peak = jnp.max(sc, axis=-1, keepdims=True)
        w = jnp.where(tri, jnp.exp(sc - peak), 0.0)
        st_m[h] = jnp.broadcast_to(peak, (tok, HD))
        st_l[h] = jnp.broadcast_to(jnp.sum(w, axis=-1, keepdims=True), (tok, HD))
        st_o[h] = jnp.dot(
            w.astype(bf16), v_ref[:, kh * HD : (kh + 1) * HD], preferred_element_type=f32
        )

    def fold(j, carry):
        @pl.when(s - j >= 0)
        def _():
            remote(k_ref, kbuf.at[j], kv_s.at[j, 0], kv_r.at[j, 0], sp=s).wait_recv()
            remote(v_ref, vbuf.at[j], kv_s.at[j, 1], kv_r.at[j, 1], sp=s).wait_recv()
            remote(gk_ref, gbuf.at[j], kv_s.at[j, 2], kv_r.at[j, 2], sp=s).wait_recv()
            for h in range(heads):
                kh = h // group
                sc = lax.dot_general(
                    q_ref[:, h * HD : (h + 1) * HD],
                    kbuf[j, :, kh * HD : (kh + 1) * HD],
                    nt,
                    preferred_element_type=f32,
                )
                sc = sc * scale + gq_ref[:, h : h + 1] - gbuf[j, h : h + 1, :]
                old = st_m[h][:, :1]
                peak = jnp.maximum(old, jnp.max(sc, axis=-1, keepdims=True))
                w = jnp.exp(sc - peak)
                fade = jnp.exp(old - peak)
                st_m[h] = jnp.broadcast_to(peak, (tok, HD))
                st_l[h] = st_l[h] * fade + jnp.sum(w, axis=-1, keepdims=True)
                st_o[h] = st_o[h] * fade + jnp.dot(
                    w.astype(bf16),
                    vbuf[j, :, kh * HD : (kh + 1) * HD],
                    preferred_element_type=f32,
                )

        return carry

    lax.fori_loop(1, S, fold, 0)

    for h in range(heads):
        a = st_o[h] / st_l[h]
        a = a * lax.rsqrt(jnp.mean(a * a, axis=-1, keepdims=True) + EPSILON)
        a = (a * hg_ref[:, h * HD : (h + 1) * HD]).astype(bf16)
        for to in range(T):
            heads_v[to % 2, (to // 2) * rows : (to // 2 + 1) * rows, h * HD : (h + 1) * HD] = a[
                to * rows : (to + 1) * rows
            ]

    chunk = 512 if D % 512 == 0 else 128

    def product(lhs, weight, put):
        for n in range(0, D, chunk):
            put(n, jnp.dot(lhs, weight[:, n : n + chunk], preferred_element_type=f32))

    def copy_a(i):
        return remote(send_a.at[i], recv_a.at[i], a_s.at[i], a_r.at[i], tp=mate)

    def copy_b(i, xo):
        return remote(
            send_b.at[i, xo], recv_b.at[i, x], b_s.at[i, xo], b_r.at[i, x], tp=at_x(xo)
        )

    def copy_b_in(i, xo):
        return remote(
            send_b.at[i, xo], recv_b.at[i, xo], b_s.at[i, xo], b_r.at[i, xo], tp=at_x(xo)
        )

    def stage_a(i, lhs_of, weight):
        def put_far(n, val):
            send_a[i, :, n : n + chunk] = val.astype(bf16)

        def put_near(n, val):
            keep[i, :, n : n + chunk] = val

        product(lhs_of(1 - c), weight, put_far)
        copy_a(i).start()
        product(lhs_of(c), weight, put_near)

    def stage_b(i):
        copy_a(i).wait_recv()
        for xo in others_x:
            at = pl.ds(pl.multiple_of(xo * rows, rows), rows)
            send_b[i, xo] = (keep[i, at, :] + recv_a[i, at, :].astype(f32)).astype(bf16)
            copy_b(i, xo).start()
        at = pl.ds(pl.multiple_of(x * rows, rows), rows)
        own[i] = keep[i, at, :] + recv_a[i, at, :].astype(f32)

    def stage_c(i):
        for xo in others_x:
            copy_b_in(i, xo).wait_recv()
        total = own[i]
        for xo in others_x:
            total = total + recv_b[i, xo].astype(f32)
        return total

    own_copies[0].wait()
    stage_a(S, lambda half_of: heads_v[half_of], wout)
    stage_b(S)
    mine = pl.ds(pl.multiple_of(x * rows, rows), rows)
    mid_all[s, c, mine, :] = layer_scale(
        ALPHA * res_ref[...].astype(f32) + stage_c(S), mg_ref[...]
    ).astype(bf16)

    def place(so, xo, co):
        return mid_all.at[so, co, pl.ds(pl.multiple_of(xo * rows, rows), rows), :]

    def mid_z(to):
        return remote(place(s, x, c), place(s, x, c), z_s.at[to], z_r.at[s], sp=to)

    def mid_z_in(so):
        return remote(place(so, x, c), place(so, x, c), z_s.at[so], z_r.at[so], sp=so)

    def mid_x(so, xo):
        return remote(place(so, x, c), place(so, x, c), x_s.at[so, xo], x_r.at[so, x], tp=at_x(xo))

    def mid_x_in(so, xo):
        return remote(
            place(so, xo, c), place(so, xo, c), x_s.at[so, xo], x_r.at[so, xo], tp=at_x(xo)
        )

    def mid_d(so, xo):
        return remote(place(so, xo, c), place(so, xo, c), d_s.at[so, xo], d_r.at[so, xo], tp=mate)

    def mid_d_in(so, xo):
        return remote(
            place(so, xo, 1 - c), place(so, xo, 1 - c), d_s.at[so, xo], d_r.at[so, xo], tp=mate
        )

    for so in others_s:
        mid_z(so).start()
    for xo in others_x:
        mid_x(s, xo).start()
    mid_d(s, x).start()
    forward_weight(0)

    def spread(so):
        mid_z_in(so).wait_recv()
        for xo in others_x:
            mid_x(so, xo).start()
        mid_d(so, x).start()

    def lift(k, carry):
        so = lax.rem(s + k, S)

        @pl.when(k + 1 < S)
        def _():
            spread(lax.rem(s + k + 1, S))

        for xo in others_x:
            mid_x_in(so, xo).wait_recv()
            mid_d(so, xo).start()
        for xo in range(X):
            mid_d_in(so, xo).wait_recv()

        @pl.when(k == 0)
        def _():
            finish_weight(0)
            own_copies[1].wait()

        for co in range(2):
            up = jnp.dot(mid_all[so, co], wup[...], preferred_element_type=f32)
            act[so, co] = jnp.square(jnp.maximum(up, 0.0)).astype(bf16)
        return carry

    lax.fori_loop(0, S, lift, 0)
    forward_weight(1)
    own_copies[2].wait()
    finish_weight(1)

    def copy_c(to):
        return remote(send_c.at[to], recv_c.at[s], c_s.at[to], c_r.at[s], sp=to)

    def copy_c_in(so):
        return remote(send_c.at[so], recv_c.at[so], c_s.at[so], c_r.at[so], sp=so)

    def lower(k, carry):
        @pl.when(k < S)
        def _():
            so = lax.rem(s + 1 + k, S)
            stage_a(so, lambda half_of: act[so, half_of], wdn)

        @pl.when(jnp.logical_and(k >= 1, k <= S))
        def _():
            stage_b(lax.rem(s + k, S))

        @pl.when(jnp.logical_and(k >= 2, k <= S))
        def _():
            so = lax.rem(s + k - 1, S)
            send_c[so] = stage_c(so).astype(bf16)
            copy_c(so).start()

        return carry

    lax.fori_loop(0, S + 1, lower, 0)
    total = stage_c(s)
    for so in others_s:
        copy_c_in(so).wait_recv()
        total = total + recv_c[so].astype(f32)
    out_ref[...] = layer_scale(
        ALPHA * mid_all[s, c, mine, :].astype(f32) + total, cg_ref[...]
    ).astype(bf16)

    for d in range(1, S):

        @pl.when(s + d < S)
        def _(d=d):
            for copy in kv_copies(d):
                copy.wait_send()

    for so in others_s:
        for m in range(2):
            z_weight(m, so).wait_send()
            for go in others_g:
                y_weight(m, so, go).wait_send()
        mid_z(so).wait_send()
        copy_c(so).wait_send()

    def drain_mid(so, carry):
        for xo in others_x:
            mid_x(so, xo).wait_send()
        for xo in range(X):
            mid_d(so, xo).wait_send()
        return carry

    lax.fori_loop(0, S, drain_mid, 0)

    def drain_sums(i, carry):
        copy_a(i).wait_send()
        for xo in others_x:
            copy_b(i, xo).wait_send()
        return carry

    lax.fori_loop(0, S + 1, drain_sums, 0)


def fused_plan(G, S, T, args):
    tok, qcols = args[1].shape
    kcols = args[2].shape[1]
    heads = args[4].shape[1]
    D = args[0].shape[1]
    ff = args[7].shape[1]
    if S < 2 or T < 2 or T % 2 or G < 2 or tok % T or D % S or ff % S:
        return None
    X, rows, dcut, fcut = T // 2, tok // T, D // S, ff // S
    if rows % 16 or dcut % 128 or fcut % 128 or D % 128 or tok % 128:
        return None
    if dcut % (16 * G) or fcut % (16 * G):
        return None
    half = X * rows
    bf16, f32 = jnp.bfloat16, jnp.float32
    buffers = [
        ((S, tok, kcols), bf16),
        ((S, tok, kcols), bf16),
        ((S, heads, tok), f32),
        ((qcols, D), bf16),
        ((D, fcut), bf16),
        ((fcut, D), bf16),
        ((2, half, qcols), bf16),
        ((S, 2, half, D), bf16),
        ((S, 2, half, fcut), bf16),
        ((S + 1, half, D), bf16),
        ((S + 1, half, D), bf16),
        ((S + 1, half, D), f32),
        ((S + 1, X, rows, D), bf16),
        ((S + 1, X, rows, D), bf16),
        ((S + 1, rows, D), f32),
        ((S, rows, D), bf16),
        ((S, rows, D), bf16),
        ((heads, tok, HD), f32),
        ((heads, tok, HD), f32),
        ((heads, tok, HD), f32),
    ]
    total = 0
    for shape, kind in buffers:
        size = jnp.dtype(kind).itemsize
        for extent in shape:
            size *= extent
        total += size
    if total > 48 * 2**20:
        return None
    sems = [
        (S, 3),
        (S, 3),
        (2, S),
        (2, S),
        (2, S, G),
        (2, S, G),
        (3,),
        (S,),
        (S,),
        (S, X),
        (S, X),
        (S, X),
        (S, X),
        (S + 1,),
        (S + 1,),
        (S + 1, X),
        (S + 1, X),
        (S,),
        (S,),
    ]
    return [pltpu.VMEM(shape, kind) for shape, kind in buffers] + [
        pltpu.SemaphoreType.DMA(shape) for shape in sems
    ]


def fused(sizes, *args):
    scratch = fused_plan(*sizes, args)
    if scratch is None:
        return shards(*args)
    res, q, k, v, gate, hg, w_out, w_up, w_down, mg, cg = args
    vmem = pl.BlockSpec(memory_space=pltpu.VMEM)
    hbm = pl.BlockSpec(memory_space=pl.ANY)
    return pl.pallas_call(
        functools.partial(layer_kernel, *sizes),
        out_shape=jax.ShapeDtypeStruct(res.shape, jnp.bfloat16),
        in_specs=[vmem] * 9 + [hbm] * 3,
        out_specs=vmem,
        scratch_shapes=scratch,
        compiler_params=pltpu.CompilerParams(
            collective_id=0, has_side_effects=True, vmem_limit_bytes=60 * 2**20
        ),
        name="layer",
    )(q, k, v, gate, gate.T, res, hg[None], mg[None], cg[None], w_out, w_up, w_down)


def solution(mesh):
    placed = (
        P(("grp", "sp", "tp"), None),
        P(("grp", "sp"), "tp"),
        P(("grp", "sp"), "tp"),
        P(("grp", "sp"), "tp"),
        P(("grp", "sp"), "tp"),
        P("tp"),
        P("tp", None),
        P("sp", "tp"),
        P("tp", "sp"),
        P(),
        P(),
    )
    sizes = (mesh.shape["grp"], mesh.shape["sp"], mesh.shape["tp"])
    return jax.shard_map(
        functools.partial(fused, sizes), mesh=mesh, in_specs=placed, out_specs=P(("grp", "sp", "tp"), None), check_vma=False
    )
```

```python
import functools

import jax
import jax.numpy as jnp
from jax import lax
from jax.experimental import pallas as pl
from jax.experimental.pallas import tpu as pltpu
from jax.sharding import PartitionSpec as P

MESH = pl.DeviceIdType.MESH

HD = 128


ALPHA = 8.0**0.25
EPSILON = 1e-05
NEG_FILL = -1e30


def layer_scale(inputs, gain_vec):
    centered = inputs - jnp.mean(inputs, axis=-1, keepdims=True)
    variance = jnp.mean(centered * centered, axis=-1, keepdims=True)
    return centered * lax.rsqrt(variance + EPSILON) * gain_vec


def shards(
    residual_in,
    query_rows,
    key_rows,
    value_rows,
    forget_cumsum,
    head_gain,
    w_out,
    w_up,
    w_down,
    mixer_gain,
    channel_gain,
):
    tok_rows = query_rows.shape[0]
    heads_here = forget_cumsum.shape[1]
    kv_here = key_rows.shape[1] // HD
    group_size = heads_here // kv_here
    score_scale = HD ** (-0.5)
    seq_index = lax.axis_index("sp")
    gate_all = lax.all_gather(forget_cumsum, "sp", axis=0, tiled=True)
    query_grid = query_rows.reshape(tok_rows, kv_here, group_size, HD)
    query_pos = seq_index * tok_rows + jnp.arange(tok_rows, dtype=jnp.int32)
    last_query = seq_index * tok_rows + tok_rows - 1
    gate_query = forget_cumsum.reshape(tok_rows, kv_here, group_size).transpose(1, 2, 0)

    def attend(carry_state, key_block, value_block, first_row):
        row_count = key_block.shape[0]

        def attend_live(live_state):
            peak_score, denom_sum, accum = live_state
            key_grid = key_block.reshape(row_count, kv_here, HD)
            value_grid = value_block.reshape(row_count, kv_here, HD)
            gate_block = lax.dynamic_slice_in_dim(gate_all, first_row, row_count, 0)
            gate_block = gate_block.reshape(row_count, kv_here, group_size).transpose(1, 2, 0)
            scores = (
                jnp.einsum(
                    "tkgd,ukd->kgtu", query_grid, key_grid, preferred_element_type=jnp.float32
                )
                * score_scale
            )
            scores = scores + gate_query[..., None] - gate_block[:, :, None, :]
            key_pos = first_row + jnp.arange(row_count, dtype=jnp.int32)
            allowed = key_pos[None, :] <= query_pos[:, None]
            scores = jnp.where(allowed, scores, NEG_FILL)
            new_peak = jnp.maximum(peak_score, jnp.max(scores, axis=-1))
            weights = jnp.where(allowed, jnp.exp(scores - new_peak[..., None]), 0.0)
            fade_factor = jnp.exp(peak_score - new_peak)
            denom_sum = denom_sum * fade_factor + jnp.sum(weights, axis=-1)
            accum = accum * fade_factor[..., None] + jnp.einsum(
                "kgtu,ukd->kgtd",
                weights.astype(jnp.bfloat16),
                value_grid,
                preferred_element_type=jnp.float32,
            )
            return (new_peak, denom_sum, accum)

        return lax.cond(
            first_row <= last_query, attend_live, lambda kept_state: kept_state, carry_state
        )

    def fold_keys(carry_state, pieces, first_row):
        key_piece, value_piece = pieces
        row_count = key_piece.shape[0]
        block_span = 1024
        if row_count > block_span and row_count % block_span == 0:

            def scan_block(scan_state, block_index):
                offset = block_index * block_span
                next_state = attend(
                    scan_state,
                    lax.dynamic_slice_in_dim(key_piece, offset, block_span, 0),
                    lax.dynamic_slice_in_dim(value_piece, offset, block_span, 0),
                    first_row + offset,
                )
                return (next_state, None)

            carry_state, unused = lax.scan(
                scan_block, carry_state, jnp.arange(row_count // block_span, dtype=jnp.int32)
            )
            return carry_state
        return attend(carry_state, key_piece, value_piece, first_row)

    fold_init = (
        jnp.full((kv_here, group_size, tok_rows), NEG_FILL, jnp.float32),
        jnp.zeros((kv_here, group_size, tok_rows), jnp.float32),
        jnp.zeros((kv_here, group_size, tok_rows, HD), jnp.float32),
    )
    peak_score, denom_sum, accum = fold_keys(
        fold_init,
        (
            lax.all_gather(key_rows, "sp", axis=0, tiled=True),
            lax.all_gather(value_rows, "sp", axis=0, tiled=True),
        ),
        jnp.int32(0),
    )
    attended = accum / denom_sum[..., None]
    normed = attended * lax.rsqrt(jnp.mean(attended * attended, axis=-1, keepdims=True) + EPSILON)
    normed = normed * head_gain.reshape(kv_here, group_size, 1, HD)
    heads_out = normed.transpose(2, 0, 1, 3).reshape(tok_rows, heads_here * HD).astype(jnp.bfloat16)
    branch = lax.psum_scatter(
        jnp.dot(heads_out, w_out, preferred_element_type=jnp.float32).astype(jnp.bfloat16),
        "tp",
        scatter_dimension=0,
        tiled=True,
    ).astype(jnp.float32)
    mid_rows = layer_scale(ALPHA * residual_in.astype(jnp.float32) + branch, mixer_gain).astype(
        jnp.bfloat16
    )
    mid_all = lax.all_gather(mid_rows, "tp", axis=0, tiled=True)
    up_full, down_full = (
        lax.all_gather(w_up, "sp", axis=0, tiled=True),
        lax.all_gather(w_down, "sp", axis=1, tiled=True),
    )
    lifted = jnp.dot(mid_all, up_full, preferred_element_type=jnp.float32)
    active = jnp.square(jax.nn.relu(lifted)).astype(jnp.bfloat16)
    lowered = lax.psum_scatter(
        jnp.dot(active, down_full, preferred_element_type=jnp.float32).astype(jnp.bfloat16),
        "tp",
        scatter_dimension=0,
        tiled=True,
    ).astype(jnp.float32)
    return layer_scale(ALPHA * mid_rows.astype(jnp.float32) + lowered, channel_gain).astype(
        jnp.bfloat16
    )


def layer_kernel(
    G,
    S,
    T,
    q_ref,
    k_ref,
    v_ref,
    gq_ref,
    gk_ref,
    res_ref,
    hg_ref,
    mg_ref,
    cg_ref,
    wout_hbm,
    wup_hbm,
    wdn_hbm,
    out_ref,
    kbuf,
    vbuf,
    gbuf,
    wout,
    wup,
    wdn,
    heads_v,
    mid_all,
    act,
    far_out,
    far_in,
    far_keep,
    far_x_out,
    far_x_in,
    far_own,
    send_a,
    recv_a,
    keep,
    send_b,
    recv_b,
    own,
    send_c,
    recv_c,
    total,
    st_m,
    st_l,
    st_o,
    kv_s,
    kv_r,
    wz_s,
    wz_r,
    wy_s,
    wy_r,
    loc,
    z_s,
    z_r,
    x_s,
    x_r,
    d_s,
    d_r,
    a_s,
    a_r,
    b_s,
    b_r,
    c_s,
    c_r,
):
    f32, bf16 = jnp.float32, jnp.bfloat16
    X = T // 2
    g, s, t = lax.axis_index("grp"), lax.axis_index("sp"), lax.axis_index("tp")
    x, c = t // 2, lax.rem(t, 2)
    mate = x * 2 + (1 - c)
    tok = q_ref.shape[0]
    heads = gq_ref.shape[1]
    kv_heads = k_ref.shape[1] // HD
    group = heads // kv_heads
    rows = tok // T
    D = res_ref.shape[1]
    dcut = D // S
    fcut = wup.shape[1]

    def remote(src, dst, ssem, rsem, **where):
        return pltpu.make_async_remote_copy(
            src_ref=src,
            dst_ref=dst,
            send_sem=ssem,
            recv_sem=rsem,
            device_id=where,
            device_id_type=MESH,
        )

    def at_x(xo):
        return xo * 2 + c

    others_s = [lax.rem(s + d, S) for d in range(1, S)]
    others_x = [lax.rem(x + d, X) for d in range(1, X)]
    others_g = [lax.rem(g + d, G) for d in range(1, G)]

    own_copies = [
        pltpu.make_async_copy(wout_hbm, wout, loc.at[0]),
        pltpu.make_async_copy(
            wup_hbm.at[:, pl.ds(pl.multiple_of(s * fcut, fcut), fcut)],
            wup.at[pl.ds(pl.multiple_of(s * dcut, dcut), dcut), :],
            loc.at[1],
        ),
        pltpu.make_async_copy(
            wdn_hbm.at[pl.ds(pl.multiple_of(s * fcut, fcut), fcut), :],
            wdn.at[s],
            loc.at[2],
        ),
    ]
    for copy in own_copies:
        copy.start()

    barrier = pltpu.get_barrier_semaphore()
    for so in others_s:
        pl.semaphore_signal(barrier, inc=1, device_id={"sp": so}, device_id_type=MESH)
    for xo in others_x:
        pl.semaphore_signal(barrier, inc=1, device_id={"tp": at_x(xo)}, device_id_type=MESH)
    pl.semaphore_signal(barrier, inc=1, device_id={"tp": mate}, device_id_type=MESH)
    for go in others_g:
        pl.semaphore_signal(barrier, inc=1, device_id={"grp": go}, device_id_type=MESH)
    pl.semaphore_wait(barrier, (S - 1) + (X - 1) + 1 + (G - 1))

    def kv_copies(d):
        to = lax.rem(s + d, S)
        return [
            remote(k_ref, kbuf.at[d], kv_s.at[d, 0], kv_r.at[d, 0], sp=to),
            remote(v_ref, vbuf.at[d], kv_s.at[d, 1], kv_r.at[d, 1], sp=to),
            remote(gk_ref, gbuf.at[d], kv_s.at[d, 2], kv_r.at[d, 2], sp=to),
        ]

    for d in range(1, S):

        @pl.when(s + d < S)
        def _(d=d):
            for copy in kv_copies(d):
                copy.start()

    uprow, dnrow = dcut // G, fcut // G

    def up_piece(so, go):
        return wup.at[pl.ds(pl.multiple_of(so * dcut + go * uprow, uprow), uprow), :]

    def dn_piece(so, go):
        return wdn.at[so, pl.ds(pl.multiple_of(go * dnrow, dnrow), dnrow), :]

    def z_weight(m, to):
        if m == 0:
            src = wup_hbm.at[
                pl.ds(pl.multiple_of(g * uprow, uprow), uprow),
                pl.ds(pl.multiple_of(to * fcut, fcut), fcut),
            ]
            dst = up_piece(s, g)
        else:
            src = wdn_hbm.at[pl.ds(pl.multiple_of(to * fcut + g * dnrow, dnrow), dnrow), :]
            dst = dn_piece(s, g)
        return remote(src, dst, wz_s.at[m, to], wz_r.at[m, s], sp=to)

    def z_weight_in(m, so):
        dst = up_piece(so, g) if m == 0 else dn_piece(so, g)
        return remote(dst, dst, wz_s.at[m, so], wz_r.at[m, so], sp=so)

    def y_weight(m, so, go):
        ref = up_piece(so, g) if m == 0 else dn_piece(so, g)
        return remote(ref, ref, wy_s.at[m, so, go], wy_r.at[m, so, g], grp=go)

    def y_weight_in(m, so, go):
        ref = up_piece(so, go) if m == 0 else dn_piece(so, go)
        return remote(ref, ref, wy_s.at[m, so, go], wy_r.at[m, so, go], grp=go)

    def start_weight(m):
        for so in others_s:
            z_weight(m, so).start()

    def forward_piece(m, so):
        z_weight_in(m, so).wait_recv()
        for go in others_g:
            y_weight(m, so, go).start()

    def finish_piece(m, so):
        for go in others_g:
            y_weight_in(m, so, go).wait_recv()

    start_weight(0)

    scale = HD ** (-0.5)
    nt = (((1,), (1,)), ((), ()))
    tri = lax.broadcasted_iota(jnp.int32, (tok, tok), 0) >= lax.broadcasted_iota(
        jnp.int32, (tok, tok), 1
    )
    for h in range(heads):
        kh = h // group
        sc = lax.dot_general(
            q_ref[:, h * HD : (h + 1) * HD],
            k_ref[:, kh * HD : (kh + 1) * HD],
            nt,
            preferred_element_type=f32,
        )
        sc = sc * scale + gq_ref[:, h : h + 1] - gk_ref[h : h + 1, :]
        sc = jnp.where(tri, sc, NEG_FILL)
        peak = jnp.max(sc, axis=-1, keepdims=True)
        w = jnp.where(tri, jnp.exp(sc - peak), 0.0)
        st_m[h] = jnp.broadcast_to(peak, (tok, HD))
        st_l[h] = jnp.broadcast_to(jnp.sum(w, axis=-1, keepdims=True), (tok, HD))
        st_o[h] = jnp.dot(
            w.astype(bf16), v_ref[:, kh * HD : (kh + 1) * HD], preferred_element_type=f32
        )

    def fold(j, carry):
        @pl.when(s - j >= 0)
        def _():
            remote(k_ref, kbuf.at[j], kv_s.at[j, 0], kv_r.at[j, 0], sp=s).wait_recv()
            remote(v_ref, vbuf.at[j], kv_s.at[j, 1], kv_r.at[j, 1], sp=s).wait_recv()
            remote(gk_ref, gbuf.at[j], kv_s.at[j, 2], kv_r.at[j, 2], sp=s).wait_recv()
            for h in range(heads):
                kh = h // group
                sc = lax.dot_general(
                    q_ref[:, h * HD : (h + 1) * HD],
                    kbuf[j, :, kh * HD : (kh + 1) * HD],
                    nt,
                    preferred_element_type=f32,
                )
                sc = sc * scale + gq_ref[:, h : h + 1] - gbuf[j, h : h + 1, :]
                old = st_m[h][:, :1]
                peak = jnp.maximum(old, jnp.max(sc, axis=-1, keepdims=True))
                w = jnp.exp(sc - peak)
                fade = jnp.exp(old - peak)
                st_m[h] = jnp.broadcast_to(peak, (tok, HD))
                st_l[h] = st_l[h] * fade + jnp.sum(w, axis=-1, keepdims=True)
                st_o[h] = st_o[h] * fade + jnp.dot(
                    w.astype(bf16),
                    vbuf[j, :, kh * HD : (kh + 1) * HD],
                    preferred_element_type=f32,
                )

        return carry

    lax.fori_loop(1, S, fold, 0)

    for h in range(heads):
        a = st_o[h] / st_l[h]
        a = a * lax.rsqrt(jnp.mean(a * a, axis=-1, keepdims=True) + EPSILON)
        a = (a * hg_ref[:, h * HD : (h + 1) * HD]).astype(bf16)
        for to in range(T):
            heads_v[to % 2, (to // 2) * rows : (to // 2 + 1) * rows, h * HD : (h + 1) * HD] = a[
                to * rows : (to + 1) * rows
            ]

    chunk = 512 if D % 512 == 0 else 128
    branch_bufs = (far_out, far_in, far_keep, far_x_out, far_x_in, far_own)

    def sum_bufs(e):
        return [ref.at[e] for ref in (send_a, recv_a, keep, send_b, recv_b, own)]

    def copy_a(i, bufs):
        return remote(bufs[0], bufs[1], a_s.at[i], a_r.at[i], tp=mate)

    def copy_b(i, bufs, xo):
        return remote(
            bufs[3].at[xo], bufs[4].at[x], b_s.at[i, xo], b_r.at[i, x], tp=at_x(xo)
        )

    def copy_b_in(i, bufs, xo):
        return remote(
            bufs[3].at[xo], bufs[4].at[xo], b_s.at[i, xo], b_r.at[i, xo], tp=at_x(xo)
        )

    def stage_b(i, bufs):
        copy_a(i, bufs).wait_recv()
        near, near_x = bufs[2], bufs[1]
        for xo in others_x:
            bufs[3][xo] = (near[xo] + near_x[xo].astype(f32)).astype(bf16)
            copy_b(i, bufs, xo).start()
        bufs[5][...] = near[x] + near_x[x].astype(f32)

    def stage_c(i, bufs):
        for xo in others_x:
            copy_b_in(i, bufs, xo).wait_recv()
        summed = bufs[5][...]
        for xo in others_x:
            summed = summed + bufs[4][xo].astype(f32)
        return summed

    def branch_half(co, put):
        for n in range(0, D, chunk):
            put(
                n,
                jnp.dot(heads_v[co], wout[:, n : n + chunk], preferred_element_type=f32).reshape(
                    X, rows, chunk
                ),
            )

    def put_far(n, val):
        far_out[:, :, n : n + chunk] = val.astype(bf16)

    def put_near(n, val):
        far_keep[:, :, n : n + chunk] = val

    own_copies[0].wait()
    branch_half(1 - c, put_far)
    copy_a(S, branch_bufs).start()
    branch_half(c, put_near)
    stage_b(S, branch_bufs)
    mine = pl.ds(pl.multiple_of(x * rows, rows), rows)
    mid_all[s, c, mine, :] = layer_scale(
        ALPHA * res_ref[...].astype(f32) + stage_c(S, branch_bufs), mg_ref[...]
    ).astype(bf16)

    def place(so, xo, co):
        return mid_all.at[so, co, pl.ds(pl.multiple_of(xo * rows, rows), rows), :]

    def mid_z(so, way):
        return remote(
            place(so, x, c), place(so, x, c), z_s.at[so, way], z_r.at[so], sp=s + (1 if way else -1)
        )

    def mid_z_in(so):
        return remote(place(so, x, c), place(so, x, c), z_s.at[so, 0], z_r.at[so], sp=so)

    def mid_x(so, xo):
        return remote(place(so, x, c), place(so, x, c), x_s.at[so, xo], x_r.at[so, x], tp=at_x(xo))

    def mid_x_in(so, xo):
        return remote(
            place(so, xo, c), place(so, xo, c), x_s.at[so, xo], x_r.at[so, xo], tp=at_x(xo)
        )

    def mid_d(so, xo):
        return remote(place(so, xo, c), place(so, xo, c), d_s.at[so, xo], d_r.at[so, xo], tp=mate)

    def mid_d_in(so, xo):
        return remote(
            place(so, xo, 1 - c), place(so, xo, 1 - c), d_s.at[so, xo], d_r.at[so, xo], tp=mate
        )

    @pl.when(s + 1 < S)
    def _():
        mid_z(s, 1).start()

    @pl.when(s > 0)
    def _():
        mid_z(s, 0).start()

    for xo in others_x:
        mid_x(s, xo).start()
    mid_d(s, x).start()
    for so in others_s:
        forward_piece(0, so)

    def spread(so):
        for xo in others_x:
            mid_x(so, xo).start()
        mid_d(so, x).start()

    def spread_left(so):
        mid_z_in(so).wait_recv()

        @pl.when(s + 1 < S)
        def _():
            mid_z(so, 1).start()

        spread(so)

    def spread_right(so):
        mid_z_in(so).wait_recv()

        @pl.when(s > 0)
        def _():
            mid_z(so, 0).start()

        spread(so)

    def lift_block(so):
        for xo in others_x:
            mid_x_in(so, xo).wait_recv()
            mid_d(so, xo).start()
        for xo in range(X):
            mid_d_in(so, xo).wait_recv()
        at = pl.ds(pl.multiple_of(so * rows, rows), rows)
        for co in range(2):
            up = jnp.dot(mid_all[so, co], wup[...], preferred_element_type=f32)
            up = jnp.square(jnp.maximum(up, 0.0)).astype(bf16)
            for xo in range(X):
                act[co, xo, at, :] = up[xo * rows : (xo + 1) * rows]

    def lift(d, carry):
        @pl.when(d + 1 < S)
        def _():
            @pl.when(s - d - 1 >= 0)
            def _():
                spread_left(s - d - 1)

            @pl.when(s + d + 1 < S)
            def _():
                spread_right(s + d + 1)

            @pl.when(d + 1 == S - 1)
            def _():
                start_weight(1)

        @pl.when(d == 0)
        def _():
            for so in others_s:
                finish_piece(0, so)
            own_copies[1].wait()

        @pl.when(s - d >= 0)
        def _():
            lift_block(s - d)

        @pl.when(jnp.logical_and(d > 0, s + d < S))
        def _():
            lift_block(s + d)

        return carry

    lax.fori_loop(0, S, lift, 0)

    def copy_c(e, to):
        return remote(send_c.at[e, to], recv_c.at[e, s], c_s.at[e, to], c_r.at[e, s], sp=to)

    def copy_c_in(e, so):
        return remote(send_c.at[e, so], recv_c.at[e, so], c_s.at[e, so], c_r.at[e, so], sp=so)

    def half_sum(e, co):
        lhs = act[co].reshape(X * S * rows, fcut)
        return jnp.dot(lhs, wdn[e], preferred_element_type=f32).reshape(X, S * rows, dcut)

    own_copies[2].wait()
    forward_piece(1, others_s[0])

    def lower(k, carry):
        @pl.when(k < S)
        def _():
            e = lax.rem(s + k, S)
            bufs = sum_bufs(e)
            bufs[0][...] = half_sum(e, 1 - c).astype(bf16)
            copy_a(e, bufs).start()
            bufs[2][...] = half_sum(e, c)
            stage_b(e, bufs)

        @pl.when(k + 2 < S)
        def _():
            forward_piece(1, lax.rem(s + k + 2, S))

        @pl.when(k >= 1)
        def _():
            e = lax.rem(s + k - 1, S)
            summed = stage_c(e, sum_bufs(e))
            own[e] = summed
            send_c[e] = summed.astype(bf16).reshape(S, rows, dcut)
            for so in others_s:
                copy_c(e, so).start()

        @pl.when(k + 1 < S)
        def _():
            finish_piece(1, lax.rem(s + k + 1, S))

        return carry

    lax.fori_loop(0, S + 1, lower, 0)
    here = pl.ds(pl.multiple_of(s * rows, rows), rows)
    for e in range(S):
        summed = own[e, here, :]
        for so in others_s:
            copy_c_in(e, so).wait_recv()
            summed = summed + recv_c[e, so].astype(f32)
        total[:, e * dcut : (e + 1) * dcut] = summed
    out_ref[...] = layer_scale(
        ALPHA * mid_all[s, c, mine, :].astype(f32) + total[...], cg_ref[...]
    ).astype(bf16)

    for d in range(1, S):

        @pl.when(s + d < S)
        def _(d=d):
            for copy in kv_copies(d):
                copy.wait_send()

    for so in others_s:
        for m in range(2):
            z_weight(m, so).wait_send()
            for go in others_g:
                y_weight(m, so, go).wait_send()
        for e in range(S):
            copy_c(e, so).wait_send()

    def drain_mid(so, carry):
        @pl.when(jnp.logical_and(so <= s, s + 1 < S))
        def _():
            mid_z(so, 1).wait_send()

        @pl.when(jnp.logical_and(so >= s, s > 0))
        def _():
            mid_z(so, 0).wait_send()

        for xo in others_x:
            mid_x(so, xo).wait_send()
        for xo in range(X):
            mid_d(so, xo).wait_send()
        return carry

    lax.fori_loop(0, S, drain_mid, 0)

    copy_a(S, branch_bufs).wait_send()
    for xo in others_x:
        copy_b(S, branch_bufs, xo).wait_send()

    def drain_sums(e, carry):
        bufs = sum_bufs(e)
        copy_a(e, bufs).wait_send()
        for xo in others_x:
            copy_b(e, bufs, xo).wait_send()
        return carry

    lax.fori_loop(0, S, drain_sums, 0)


def fused_plan(G, S, T, args):
    tok, qcols = args[1].shape
    kcols = args[2].shape[1]
    heads = args[4].shape[1]
    D = args[0].shape[1]
    ff = args[7].shape[1]
    if S < 2 or T < 2 or T % 2 or G < 2 or tok % T or D % S or ff % S:
        return None
    X, rows, dcut, fcut = T // 2, tok // T, D // S, ff // S
    if rows % 16 or dcut % 128 or fcut % 128 or D % 128 or tok % 128:
        return None
    if dcut % (16 * G) or fcut % (16 * G):
        return None
    half = X * rows
    bf16, f32 = jnp.bfloat16, jnp.float32
    buffers = [
        ((S, tok, kcols), bf16),
        ((S, tok, kcols), bf16),
        ((S, heads, tok), f32),
        ((qcols, D), bf16),
        ((D, fcut), bf16),
        ((S, fcut, dcut), bf16),
        ((2, half, qcols), bf16),
        ((S, 2, half, D), bf16),
        ((2, X, S * rows, fcut), bf16),
        ((X, rows, D), bf16),
        ((X, rows, D), bf16),
        ((X, rows, D), f32),
        ((X, rows, D), bf16),
        ((X, rows, D), bf16),
        ((rows, D), f32),
        ((S, X, S * rows, dcut), bf16),
        ((S, X, S * rows, dcut), bf16),
        ((S, X, S * rows, dcut), f32),
        ((S, X, S * rows, dcut), bf16),
        ((S, X, S * rows, dcut), bf16),
        ((S, S * rows, dcut), f32),
        ((S, S, rows, dcut), bf16),
        ((S, S, rows, dcut), bf16),
        ((rows, D), f32),
        ((heads, tok, HD), f32),
        ((heads, tok, HD), f32),
        ((heads, tok, HD), f32),
    ]
    total = 0
    for shape, kind in buffers:
        size = jnp.dtype(kind).itemsize
        for extent in shape:
            size *= extent
        total += size
    if total > 48 * 2**20:
        return None
    sems = [
        (S, 3),
        (S, 3),
        (2, S),
        (2, S),
        (2, S, G),
        (2, S, G),
        (3,),
        (S, 2),
        (S,),
        (S, X),
        (S, X),
        (S, X),
        (S, X),
        (S + 1,),
        (S + 1,),
        (S + 1, X),
        (S + 1, X),
        (S, S),
        (S, S),
    ]
    return [pltpu.VMEM(shape, kind) for shape, kind in buffers] + [
        pltpu.SemaphoreType.DMA(shape) for shape in sems
    ]


def fused(sizes, *args):
    scratch = fused_plan(*sizes, args)
    if scratch is None:
        return shards(*args)
    res, q, k, v, gate, hg, w_out, w_up, w_down, mg, cg = args
    vmem = pl.BlockSpec(memory_space=pltpu.VMEM)
    hbm = pl.BlockSpec(memory_space=pl.ANY)
    return pl.pallas_call(
        functools.partial(layer_kernel, *sizes),
        out_shape=jax.ShapeDtypeStruct(res.shape, jnp.bfloat16),
        in_specs=[vmem] * 9 + [hbm] * 3,
        out_specs=vmem,
        scratch_shapes=scratch,
        compiler_params=pltpu.CompilerParams(
            collective_id=0, has_side_effects=True, vmem_limit_bytes=60 * 2**20
        ),
        name="layer",
    )(q, k, v, gate, gate.T, res, hg[None], mg[None], cg[None], w_out, w_up, w_down)


def solution(mesh):
    placed = (
        P(("grp", "sp", "tp"), None),
        P(("grp", "sp"), "tp"),
        P(("grp", "sp"), "tp"),
        P(("grp", "sp"), "tp"),
        P(("grp", "sp"), "tp"),
        P("tp"),
        P("tp", None),
        P("sp", "tp"),
        P("tp", "sp"),
        P(),
        P(),
    )
    sizes = (mesh.shape["grp"], mesh.shape["sp"], mesh.shape["tp"])
    return jax.shard_map(
        functools.partial(fused, sizes), mesh=mesh, in_specs=placed, out_specs=P(("grp", "sp", "tp"), None), check_vma=False
    )
```
